32 devices in a mesh: ep: 32 (over z, y, x, core).
Axes of the slice: x: 2, y: 2, z: 4, core: 2. Of those that a mesh axis runs over, the one named last changes fastest.
Arguments:
- tokens: bfloat16 [2048, 2048], P('ep'), may hold values from -6 to 6
- conv_state: bfloat16 [2048, 3, 1024], P('ep'), may hold values from -6 to 6
- recur_state: float32 [2048, 1024], P('ep'), may hold values from -6 to 6
- w_branch: bfloat16 [2048, 1024], replicated, may hold values from -0.125 to 0.125
- w_gate: bfloat16 [2048, 1024], replicated, may hold values from -0.125 to 0.125
- conv_taps: float32 [4, 1024], replicated, may hold values from -3 to 3
- rate_blocks: bfloat16 [16, 64, 64], replicated, may hold values from -0.75 to 0.75
- input_blocks: bfloat16 [16, 64, 64], replicated, may hold values from -0.75 to 0.75
- decay_param: float32 [1024], replicated, may hold values from 1.5 to 6.5
- w_mix: bfloat16 [1024, 2048], replicated, may hold values from -0.1875 to 0.1875
- gain_pre: float32 [2048], replicated, may hold values from 0.1 to 1.9
- gain_post: float32 [2048], replicated, may hold values from 0.1 to 1.9
- gain_ffn: float32 [2048], replicated, may hold values from 0.1 to 1.9
- gain_out: float32 [2048], replicated, may hold values from 0.1 to 1.9
- routes: int32 [2048, 2], P('ep'), may hold values from 0 to 31, all different within a row; in each aligned block of 64 rows (0 to 63, 64 to 127, ...) at most 12 rows name the same one
- affinity: float32 [2048, 2], P('ep'), may hold values from 0.05 to 1
- w_expert_gate: bfloat16 [32, 2048, 512], P('ep'), may hold values from -0.125 to 0.125
- w_expert_up: bfloat16 [32, 2048, 512], P('ep'), may hold values from -0.125 to 0.125
- w_expert_down: bfloat16 [32, 512, 2048], P('ep'), may hold values from -0.25 to 0.25
Outputs:
- layer_out: bfloat16 [2048, 2048], P('ep')
- conv_next: bfloat16 [2048, 3, 1024], P('ep')
- state_next: float32 [2048, 1024], P('ep')
The draws below stay inside these ranges and needn't reach their ends.
Inputs may be any that keep to these rules, and one draw needn't show every extreme that they name: `routes`: each row names 2 different experts. Among the 64 rows of one device no expert is named more than 12 times, and in every draw some device names some expert exactly 12 times.
All inputs are finite; a program needn't handle non-finite values.
Results may differ from the reference program's by a relative error of at most 0.014.
Values may be sent and summed in bfloat16 or wider, within the bound.
A program may use at most 128 MiB of HBM per device.

```python
import math
import jax
import jax.numpy as jnp
import numpy as np
from jax import lax

D = 2048
BW = 1024
NB = 16
BS = 64
TAPS = 4
FF = 512
TOP_K = 2
SEQ_DEV = 64
TOKENS = 2048
EXPERTS = 32
CAP = 12
LIMIT = 64


def block_scale(own_key, extent, cuts, least, largest):
    def one(position, parts):
        heights = jax.random.uniform(jax.random.fold_in(jax.random.fold_in(own_key, 6), position), (parts,), jnp.float32, least / len(cuts), largest / len(cuts))
        return jnp.repeat(jnp.exp(heights), extent[position] // parts).reshape((-1,) + (1,) * (len(extent) - position - 1))

    factor_of = one(*cuts[0])
    for cut in cuts[1:]:
        factor_of = factor_of * one(*cut)
    return factor_of


def deal_out(key, own, number, rows, count, top, reach, slope):
    sequence = jax.random.permutation(key, count)
    packed, common = portions_of(count, rows * top, reach, slope, True), portions_of(count, rows * top, reach, slope, False)
    places = jnp.arange(count)

    def named(lengths, offset_by):
        used = int((lengths > 0).sum())
        fixed = max(1, used // 4)
        passed = fixed + (places - fixed + offset_by * (used - fixed)) % max(1, count - fixed)
        return jnp.zeros((count,), jnp.int32).at[sequence[jnp.where(places < fixed, places, passed)]].set(jnp.asarray(lengths, jnp.int32))

    lengths = jnp.where(number % 4 == 0, named(packed, number // 4), named(common, number - number // 4 - 1))
    mixed = jax.random.permutation(jax.random.fold_in(own, 3), count)
    donor, sink = mixed[0:count // 2 * 2:2], mixed[1:count // 2 * 2:2]
    margin = jnp.minimum(lengths[donor] - 1, reach - lengths[sink]) // 2
    margin = jnp.where((donor == sequence[0]) | (sink == sequence[0]) | (lengths[sink] == 0), 0, jnp.maximum(margin, 0))
    passed = jax.random.randint(jax.random.fold_in(own, 4), (count // 2,), 0, 1 << 20) % (margin + 1)
    lengths = lengths.at[donor].add(-passed).at[sink].add(passed)
    labels = jnp.searchsorted(jnp.cumsum(lengths), jnp.arange(rows * top), side="right").astype(jnp.int32)
    listing = labels.reshape(top, rows).T
    listing = listing[jax.random.permutation(jax.random.fold_in(own, 1), rows)]
    offset_by = jax.random.randint(jax.random.fold_in(own, 2), (rows, 1), 0, top)
    return jnp.take_along_axis(listing, (jnp.arange(top)[None, :] + offset_by) % top, axis=1)


def portions_of(count, total, reach, skew, full):
    portions = [(1 << 20) // math.isqrt(standing ** skew) + 1 for standing in range(1, count + 1)]
    largest = reach if full else min(reach, max(-(-total // count), total * portions[0] // sum(portions)))
    least = 1 if total - largest >= count - 1 else 0
    given, surplus = [largest] + [least] * (count - 1), total - largest - least * (count - 1)
    while surplus > 0:
        movable = [i for i in range(1, count) if given[i] < largest] or [i for i in range(1, count) if given[i] < reach]
        whole, left = sum([portions[i] for i in movable]), surplus
        for i in movable:
            more = min(reach - given[i], max(1, left * portions[i] // whole), surplus)
            given[i] = given[i] + more
            surplus = surplus - more
    return np.array(given)


def gaussian(own_key, dims, deviation, limit, shards=(), kind=jnp.bfloat16):
    values = jax.random.normal(own_key, dims, jnp.float32) * deviation
    if len(shards) > 0:
        values = block_scale(own_key, dims, shards, -0.22, 0.18) * values
    return jnp.clip(values, min=-limit, max=limit).astype(kind)


def setup_inputs(seed: int = 0) -> dict:
    streams_of = jax.random.split(jax.random.key(seed), 20)
    tokens = gaussian(streams_of[0], (TOKENS, D), 1.0, 6.0, ((0, 32),))
    conv_state = gaussian(streams_of[1], (TOKENS, TAPS - 1, BW), 1.0, 6.0, ((0, 32),))
    recur_state = gaussian(streams_of[2], (TOKENS, BW), 1.0, 6.0, ((0, 32),), jnp.float32)
    w_branch = gaussian(streams_of[3], (D, BW), D ** -0.5, 0.125)
    w_gate = gaussian(streams_of[4], (D, BW), D ** -0.5, 0.125)
    conv_taps = gaussian(streams_of[5], (TAPS, BW), TAPS ** -0.5, 3.0, (), jnp.float32)
    rate_blocks = gaussian(streams_of[6], (NB, BS, BS), BS ** -0.5, 0.75)
    input_blocks = gaussian(streams_of[7], (NB, BS, BS), BS ** -0.5, 0.75)
    decay_param = jnp.clip(jax.random.uniform(streams_of[8], (BW,), jnp.float32, 1.5, 6.5), 1.5, 6.5)
    w_mix = gaussian(streams_of[9], (BW, D), BW ** -0.5, 0.1875)
    gain_pre = jnp.clip(1.0 + 0.18 * jax.random.normal(streams_of[10], (D,), jnp.float32), 0.1, 1.9)
    gain_post = jnp.clip(1.0 + 0.18 * jax.random.normal(streams_of[11], (D,), jnp.float32), 0.1, 1.9)
    gain_ffn = jnp.clip(1.0 + 0.18 * jax.random.normal(streams_of[12], (D,), jnp.float32), 0.1, 1.9)
    gain_out = jnp.clip(1.0 + 0.18 * jax.random.normal(streams_of[13], (D,), jnp.float32), 0.1, 1.9)
    routes_keys = jax.random.split(jax.random.fold_in(streams_of[14], 1), TOKENS // SEQ_DEV)
    routes_turns = jax.random.permutation(jax.random.fold_in(streams_of[14], 3), TOKENS // SEQ_DEV)
    routes = jax.vmap(lambda own, number: deal_out(jax.random.fold_in(streams_of[14], 2), own, number, SEQ_DEV, EXPERTS, TOP_K, CAP, 2))(routes_keys, routes_turns).reshape((TOKENS, TOP_K))
    affinity = jnp.clip(jnp.exp(math.log(1.0) - 2.9957323 * jax.random.uniform(streams_of[15], (TOKENS, TOP_K), jnp.float32) ** block_scale(streams_of[15], (TOKENS, TOP_K), ((0, 32),), -0.2, 0.2)), 0.05, 1.0)
    w_expert_gate = gaussian(streams_of[16], (EXPERTS, D, FF), D ** -0.5, 0.125, ((0, 32),))
    w_expert_up = gaussian(streams_of[17], (EXPERTS, D, FF), D ** -0.5, 0.125, ((0, 32),))
    w_expert_down = gaussian(streams_of[18], (EXPERTS, FF, D), FF ** -0.5, 0.25, ((0, 32),))
    return dict(tokens=tokens, conv_state=conv_state, recur_state=recur_state, w_branch=w_branch, w_gate=w_gate, conv_taps=conv_taps, rate_blocks=rate_blocks, input_blocks=input_blocks, decay_param=decay_param, w_mix=w_mix, gain_pre=gain_pre, gain_post=gain_post, gain_ffn=gain_ffn, gain_out=gain_out, routes=routes, affinity=affinity, w_expert_gate=w_expert_gate, w_expert_up=w_expert_up, w_expert_down=w_expert_down)


epsilon = 1e-06
gate_scale = 8.0

def norm_rows(values, gain_vec):
    floats = values.astype(jnp.float32)
    inv_scale = lax.rsqrt(lax.optimization_barrier(jnp.mean(floats * floats, axis=-1, keepdims=True)) + epsilon)
    return floats * inv_scale * gain_vec.astype(jnp.float32)

def recurrence(tokens, conv_state, recur_state, w_branch, w_gate, conv_taps, rate_blocks, input_blocks, decay_param, w_mix, gain_pre, gain_post):
    normed = norm_rows(tokens, gain_pre).astype(jnp.bfloat16)
    branch = jnp.dot(normed, w_branch, preferred_element_type=jnp.float32).astype(jnp.bfloat16)
    gate_act = jnp.dot(normed, w_gate, preferred_element_type=jnp.float32).astype(jnp.bfloat16)
    window = jnp.concatenate([conv_state, branch[:, None, :]], axis=1)
    convolved = lax.optimization_barrier(jnp.sum(window.astype(jnp.float32) * conv_taps.astype(jnp.float32)[None], axis=1))
    row_count, branch_width = convolved.shape
    blocks = rate_blocks.shape[0]
    pieces = convolved.reshape(row_count, blocks, branch_width // blocks)
    rate_gate = jax.nn.sigmoid(jnp.einsum('snc,ncd->snd', pieces, rate_blocks.astype(jnp.float32)).reshape(row_count, branch_width))
    inflow = jax.nn.sigmoid(jnp.einsum('snc,ncd->snd', pieces, input_blocks.astype(jnp.float32)).reshape(row_count, branch_width))
    log_decay = -gate_scale * rate_gate * jax.nn.softplus(-decay_param.astype(jnp.float32))
    state_next = jnp.exp(log_decay) * recur_state + jnp.sqrt(-jnp.expm1(2.0 * log_decay)) * (inflow * convolved)
    merged = (state_next * jax.nn.gelu(gate_act.astype(jnp.float32))).astype(jnp.bfloat16)
    mix_out = jnp.dot(merged, w_mix, preferred_element_type=jnp.float32).astype(jnp.bfloat16)
    residual = tokens.astype(jnp.float32) + norm_rows(mix_out, gain_post)
    return (residual, window[:, 1:, :], state_next)

def expert_rows(bundle):
    row_block, gate_w, up_w, down_w = bundle
    gate_part = jnp.dot(row_block, gate_w, preferred_element_type=jnp.float32)
    up_part = jnp.dot(row_block, up_w, preferred_element_type=jnp.float32)
    hidden = (jax.nn.silu(gate_part) * up_part).astype(jnp.bfloat16)
    return jnp.dot(hidden, down_w, preferred_element_type=jnp.float32).astype(jnp.bfloat16)

def reference(tokens, conv_state, recur_state, w_branch, w_gate, conv_taps, rate_blocks, input_blocks, decay_param, w_mix, gain_pre, gain_post, gain_ffn, gain_out, routes, affinity, w_expert_gate, w_expert_up, w_expert_down):
    residual, conv_next, state_next = recurrence(tokens, conv_state, recur_state, w_branch, w_gate, conv_taps, rate_blocks, input_blocks, decay_param, w_mix, gain_pre, gain_post)
    ffn_in = norm_rows(residual, gain_ffn).astype(jnp.bfloat16)
    flat_routes = routes.reshape(-1).astype(jnp.int32)
    onehot = (flat_routes[:, None] == jnp.arange(EXPERTS, dtype=jnp.int32)[None, :]).astype(jnp.int32)
    rank_all = lax.optimization_barrier(jnp.sum(jnp.cumsum(onehot, axis=0) * onehot, axis=1)) - 1
    kept_rows = rank_all < LIMIT
    target = jnp.where(kept_rows, flat_routes * LIMIT + rank_all, EXPERTS * LIMIT).astype(jnp.int32)
    repeated = jnp.repeat(ffn_in, TOP_K, axis=0)
    buffer = jnp.zeros((EXPERTS * LIMIT + 1, D), jnp.bfloat16).at[target].set(repeated)
    grouped = buffer[:EXPERTS * LIMIT].reshape(EXPERTS, LIMIT, D)
    outputs = lax.map(expert_rows, (grouped, w_expert_gate, w_expert_up, w_expert_down))
    out_table = jnp.concatenate([outputs.reshape(EXPERTS * LIMIT, D), jnp.zeros((1, D), jnp.bfloat16)], axis=0)
    picked = jnp.take(out_table, target, axis=0).astype(jnp.float32).reshape(TOKENS, TOP_K, D)
    weights = affinity / lax.optimization_barrier(jnp.sum(affinity, axis=1, keepdims=True))
    combined = lax.optimization_barrier(jnp.sum(weights[:, :, None] * picked, axis=1))
    layer_out = (residual + norm_rows(combined, gain_out)).astype(jnp.bfloat16)
    return (layer_out, conv_next, state_next)
```

```python
import functools

import jax
import jax.numpy as jnp
from jax import lax
from jax.experimental import pallas as pl
from jax.experimental.pallas import tpu as pltpu
from jax.sharding import PartitionSpec as P

epsilon = 1e-06
gate_scale = 8.0
planes = 4
cores = 2
steps = 4
tile = 256
lane = 128

f32, bf16 = jnp.float32, jnp.bfloat16


def rms(values, gain):
    return values * lax.rsqrt(jnp.mean(values * values, axis=-1, keepdims=True) + epsilon) * gain


def iota(shape, dim):
    return lax.broadcasted_iota(jnp.int32, shape, dim)


class Exchange:
    def __init__(self, n, refs):
        (
            self.zb, self.ob, self.ib, self.pb, self.sb, self.lo, self.hi, self.m1, self.m2,
            self.zs, self.zr, self.zds, self.zdr, self.os, self.ir,
            self.ps, self.pr, self.pds, self.pdr, self.ss, self.lr, self.hr,
        ) = refs
        self.n = n
        self.group = n // planes
        self.chips = self.group // cores
        me = lax.axis_index("ep")
        self.me = me
        self.plane, column = me // self.group, lax.rem(me, self.group)
        self.chip, self.core = column // cores, lax.rem(column, cores)
        self.partner = me - self.core + lax.rem(self.core + 1, cores)

    def rcopy(self, src, dst, send, recv, device):
        return pltpu.make_async_remote_copy(
            src_ref=src, dst_ref=dst, send_sem=send, recv_sem=recv,
            device_id={"ep": device}, device_id_type=pl.DeviceIdType.MESH,
        )

    def put_z(self, j, rows):
        self.zb[j, self.core, self.plane] = rows
        for up in (True, False):

            @pl.when(self.plane + 1 < planes if up else self.plane > 0)
            def _():
                self.z_copy(j, self.plane, up).start()

    def put_p(self, j, rows):
        self.pb[j, self.core, self.chip] = rows
        for d in range(1, self.chips):
            self.p_copy(j, d).start()

    def z_copy(self, j, origin, up):
        spot = self.zb.at[j, self.core, origin]
        return self.rcopy(
            spot, spot, self.zs.at[j, origin + (planes if up else 0)], self.zr.at[j, origin],
            lax.rem(self.me + (self.group if up else self.n - self.group), self.n),
        )

    def z_hop(self, j, h):
        for up in (True, False):
            origin = self.plane - h if up else self.plane + h

            @pl.when(origin >= 0 if up else origin < planes)
            def _():
                self.z_copy(j, origin, up).wait_recv()

                @pl.when(self.plane + 1 < planes if up else self.plane > 0)
                def _():
                    self.z_copy(j, origin, up).start()

    def z_share_copy(self, j, landing):
        core = lax.rem(self.core + 1, cores) if landing else self.core
        spot = self.zb.at[j, core]
        return self.rcopy(spot, spot, self.zds.at[j], self.zdr.at[j], self.partner)

    def z_share(self, j):
        self.z_share_copy(j, False).start()

    def beside(self, d):
        other = lax.rem(self.chip + d, self.chips)
        return other, self.plane * self.group + other * cores + self.core

    def o_copy(self, j, d):
        other, device = self.beside(d)
        return self.rcopy(
            self.ob.at[j, other], self.ib.at[j, self.chip], self.os.at[j], self.ir.at[j], device
        )

    def o_all(self, j):
        most = pl.ds(0, self.chips - 1)
        return self.rcopy(
            self.ob.at[j, most], self.ib.at[j, most], self.os.at[j], self.ir.at[j], self.partner
        )

    def z_mix(self, j):
        self.z_share_copy(j, True).wait_recv()
        rows, width = self.zb.shape[-2:]
        mixed = jnp.dot(
            self.m1[...], self.zb[j].reshape(-1, width), preferred_element_type=f32
        ).astype(bf16)
        self.ob[j] = mixed.reshape(self.chips, rows, width)
        for d in range(1, self.chips):
            self.o_copy(j, d).start()
        self.ib[j, self.chip] = self.ob[j, self.chip]

    def z_take(self, j):
        self.o_all(j).wait_recv()
        total = self.ib[j, 0].astype(f32)
        for chip in range(1, self.chips):
            total = total + self.ib[j, chip].astype(f32)
        return total

    def p_copy(self, j, d):
        _, device = self.beside(d)
        spot = self.pb.at[j, self.core, self.chip]
        return self.rcopy(spot, spot, self.ps.at[j], self.pr.at[j], device)

    def p_all(self, j):
        spot = self.pb.at[j, self.core, pl.ds(0, self.chips - 1)]
        return self.rcopy(spot, spot, self.ps.at[j], self.pr.at[j], self.partner)

    def p_share_copy(self, j, landing):
        core = lax.rem(self.core + 1, cores) if landing else self.core
        spot = self.pb.at[j, core]
        return self.rcopy(spot, spot, self.pds.at[j], self.pdr.at[j], self.partner)

    def p_share(self, j):
        self.p_all(j).wait_recv()
        self.p_share_copy(j, False).start()

    def s_copy(self, j, q, up):
        landing, recv = (self.lo, self.lr) if up else (self.hi, self.hr)
        return self.rcopy(
            self.sb.at[j, q], landing.at[j, q], self.ss.at[j], recv.at[j, q],
            lax.rem(self.me + (self.group if up else self.n - self.group), self.n),
        )

    def s_all(self, j):
        most = pl.ds(0, planes - 1)
        return self.rcopy(
            self.sb.at[j, most], self.lo.at[j, most], self.ss.at[j], self.lr.at[j, 0], self.partner
        )

    def p_mix(self, j):
        self.p_share_copy(j, True).wait_recv()
        rows, width = self.pb.shape[-2:]
        mixed = jnp.dot(
            self.m2[...], self.pb[j].reshape(-1, width), preferred_element_type=f32
        ).astype(bf16)
        self.sb[j] = mixed.reshape(planes, rows, width)
        self.p_hop(j, 0)

    def p_hop(self, j, h):
        def send(q, up):
            if h > 0:
                copy = self.s_copy(j, q, up)
                copy.wait_recv()
                landing = self.lo if up else self.hi
                self.sb[j, q] = (self.sb[j, q].astype(f32) + landing[j, q].astype(f32)).astype(bf16)
            self.s_copy(j, q, up).start()

        @pl.when(self.plane == h)
        def _():
            for q in range(planes - 1, h, -1):
                send(q, True)

        @pl.when(self.plane == planes - 1 - h)
        def _():
            for q in range(planes - 1 - h):
                send(q, False)

    def p_take(self, j, total):
        q = self.plane
        total[...] = self.sb[j, q].astype(f32)
        for up in (True, False):

            @pl.when(q > 0 if up else q + 1 < planes)
            def _():
                self.s_copy(j, q, up).wait_recv()
                total[...] += (self.lo if up else self.hi)[j, q].astype(f32)

    def run(self, fill, take_z, take_p):
        z, p = self.z_hop, self.p_hop
        assert steps == 4 and planes == 4
        z(0, 1); z(1, 1)
        fill()
        self.p_share(0)
        z(2, 1); z(3, 1)
        self.p_mix(0)
        z(0, 2); z(1, 2)
        self.p_share(1)
        z(2, 2); z(3, 2)
        self.p_mix(1)
        self.p_share(2)
        p(0, 1)
        z(0, 3); self.z_share(0)
        z(1, 3); self.z_share(1)
        self.p_mix(2)
        self.p_share(3)
        z(2, 3); self.z_share(2)
        self.z_mix(0)
        z(3, 3); self.z_share(3)
        p(1, 1)
        self.p_mix(3)
        self.z_mix(1)
        p(0, 2)
        self.z_mix(2)
        p(2, 1)
        self.z_mix(3)
        p(1, 2)
        p(3, 1)
        p(2, 2)
        take_z(0); take_z(1)
        p(3, 2)
        take_z(2); take_z(3)
        for j in range(steps):
            take_p(j)

    def drain(self):
        for j in range(steps):
            for up in (True, False):
                open_end = self.plane + 1 < planes if up else self.plane > 0
                for h in range(planes):
                    origin = self.plane - h if up else self.plane + h

                    @pl.when(open_end & (origin >= 0 if up else origin < planes))
                    def _():
                        self.z_copy(j, origin, up).wait_send()

            self.z_share_copy(j, False).wait_send()
            self.p_share_copy(j, False).wait_send()
            self.o_all(j).wait_send()
            self.p_all(j).wait_send()
            self.s_all(j).wait_send()


def exchange_scratch(n, rows, width):
    group = n // planes
    chips = group // cores
    part = width // (2 * steps)
    dma = lambda *count: pltpu.SemaphoreType.DMA(count)
    held = lambda *lead: pltpu.VMEM((steps, *lead, rows, part), bf16)
    return [
        held(cores, planes), held(chips), held(chips), held(cores, chips),
        held(planes), held(planes), held(planes),
        pltpu.VMEM((chips * rows, cores * planes * rows), bf16),
        pltpu.VMEM((planes * rows, cores * chips * rows), bf16),
        dma(steps, 2 * planes), dma(steps, planes), dma(steps), dma(steps), dma(steps), dma(steps),
        dma(steps), dma(steps), dma(steps), dma(steps), dma(steps),
        dma(steps, planes), dma(steps, planes),
    ]


exchange_refs = 22
input_count = 19
output_count = 3


def layer_kernel(n, limit, top, *refs):
    (
        tokens_h, conv_h, recur_h, wb_h, wg_h, taps_h, rate_h, input_h, decay_h, wm_h,
        g_pre_h, g_post_h, g_ffn_h, g_out_h, routes_h, affinity_h, eg_h, eu_h, ed_h,
    ) = refs[:input_count]
    out_h, branch_h, state_h = refs[input_count : input_count + output_count]
    refs = refs[input_count + output_count :]
    (
        tokens, conv_in, recur, wb, wg, taps, rate_b, input_b, decay_p, wm,
        g_pre, g_post, g_ffn, g_out, routes, affinity, eg, eu, ed,
    ) = refs[:input_count]
    refs = refs[input_count:]
    first = Exchange(n, refs[:exchange_refs])
    second = Exchange(n, refs[exchange_refs : 2 * exchange_refs])
    (
        out, branch_out, state_out, normed, gate_act, merged, mix, residual, message, mall,
        codes, base, share_at, sums_g, sums_u, total, hidden,
        load_sem, tile_sem, save_sem, ms, mr,
    ) = refs[2 * exchange_refs :]
    me, group, chips = first.me, first.group, first.chips
    plane, chip, core = first.plane, first.chip, first.core
    rows, width = tokens.shape
    channels = recur.shape[1]
    block = rate_b.shape[1]
    part = width // (2 * steps)
    wide = width // tile
    narrow = channels // tile

    sources = dict(
        tokens=(tokens_h, tokens), g_pre=(g_pre_h, g_pre), routes=(routes_h, routes),
        affinity=(affinity_h, affinity), conv=(conv_h, conv_in), taps=(taps_h, taps),
        rate=(rate_h, rate_b), input=(input_h, input_b), decay=(decay_h, decay_p),
        recur=(recur_h, recur), g_post=(g_post_h, g_post), g_ffn=(g_ffn_h, g_ffn),
        g_out=(g_out_h, g_out), eg=(eg_h.at[0], eg), eu=(eu_h.at[0], eu), ed=(ed_h.at[0], ed),
    )
    load = {
        name: pltpu.make_async_copy(src, dst, load_sem.at[k])
        for k, (name, (src, dst)) in enumerate(sources.items())
    }

    def strip(src, dst, t, k):
        cols = pl.ds(t * tile, tile)
        return pltpu.make_async_copy(src.at[:, cols], dst.at[:, cols], tile_sem.at[k])

    strips_b = [strip(wb_h, wb, t, t) for t in range(narrow)]
    strips_g = [strip(wg_h, wg, t, narrow + t) for t in range(narrow)]
    strips_m = [strip(wm_h, wm, t, 2 * narrow + t) for t in range(wide)]
    barrier = pltpu.get_barrier_semaphore()

    for name in ("tokens", "g_pre", "routes", "affinity"):
        load[name].start()
    for copy in strips_b:
        copy.start()

    @pl.loop(1, n)
    def _(d):
        pl.semaphore_signal(barrier, inc=1, device_id={"ep": lax.rem(me + d, n)})

    for copy in strips_g:
        copy.start()
    for name in ("conv", "taps", "rate", "input", "decay", "recur"):
        load[name].start()
    for copy in strips_m:
        copy.start()
    for name in ("g_post", "g_ffn", "g_out", "eg", "eu", "ed"):
        load[name].start()

    def lanes(k):
        return pl.ds(pl.multiple_of(k * lane, lane), lane)

    def message_copy(d, landing):
        device = lax.rem(me + d, n)
        spot = device if landing else me
        return pltpu.make_async_remote_copy(
            src_ref=message, dst_ref=mall.at[:, lanes(spot)], send_sem=ms.at[device],
            recv_sem=mr.at[spot], device_id={"ep": device},
            device_id_type=pl.DeviceIdType.MESH,
        )

    message[...] = jnp.full(message.shape, -1.0, f32)
    load["routes"].wait()
    load["affinity"].wait()
    message[:top, :rows] = routes[...].astype(f32)
    message[top : 2 * top, :rows] = affinity[...]
    mall[:, lanes(me)] = message[...]
    load["tokens"].wait()
    load["g_pre"].wait()
    normed[...] = rms(tokens[...].astype(f32), g_pre[...]).astype(bf16)

    def project(copies, weights, t):
        copies[t].wait()
        return jnp.dot(
            normed[...], weights[:, t * tile : (t + 1) * tile], preferred_element_type=f32
        ).astype(bf16)

    for t in range(narrow):
        branch_out[:, t * tile : (t + 1) * tile] = project(strips_b, wb, t)
    save_branch = pltpu.make_async_copy(branch_out, branch_h, save_sem.at[0])
    save_branch.start()
    pl.semaphore_wait(barrier, n - 1)

    @pl.loop(1, n)
    def _(d):
        message_copy(d, False).start()

    for t in range(narrow):
        gate_act[:, t * tile : (t + 1) * tile] = project(strips_g, wg, t)
    for name in ("conv", "taps", "rate", "input", "decay", "recur"):
        load[name].wait()

    same = iota((tile, tile), 0) // block == iota((tile, tile), 1) // block

    def spread(ref, t):
        piece = ref[pl.ds(t * tile, tile), :].astype(f32)
        return jnp.where(same, jnp.concatenate([piece] * (tile // block), axis=1), 0.0).astype(bf16)

    past = conv_in.shape[0]
    for t in range(narrow):
        cols = slice(t * tile, (t + 1) * tile)
        conv = branch_out[:, cols].astype(f32) * taps[past : past + 1, cols]
        for k in range(past):
            conv = conv + conv_in[k, :, cols].astype(f32) * taps[k : k + 1, cols]
        conv16 = conv.astype(bf16)
        rate = jax.nn.sigmoid(jnp.dot(conv16, spread(rate_b, t), preferred_element_type=f32))
        inflow = jax.nn.sigmoid(jnp.dot(conv16, spread(input_b, t), preferred_element_type=f32))
        log_decay = rate * (-gate_scale * jax.nn.softplus(-decay_p[:, cols]))
        decay = jnp.exp(log_decay)
        rest = -jnp.tanh(log_decay) * (decay * decay + 1.0)
        state = decay * recur[:, cols] + jnp.sqrt(rest) * (inflow * conv)
        state_out[:, cols] = state
        merged[:, cols] = (state * jax.nn.gelu(gate_act[:, cols].astype(f32))).astype(bf16)
    save_state = pltpu.make_async_copy(state_out, state_h, save_sem.at[1])
    save_state.start()

    for t in range(wide):
        strips_m[t].wait()
        cols = slice(t * tile, (t + 1) * tile)
        mix[:, cols] = (
            jnp.dot(merged[...], wm[:, cols], preferred_element_type=f32).astype(bf16).astype(f32)
        )
    for name in ("g_post", "g_ffn", "g_out"):
        load[name].wait()
    residual[...] = tokens[...].astype(f32) + rms(mix[...], g_post[...])
    ffn = rms(residual[...], g_ffn[...]).astype(bf16)

    def feature(half, j):
        start = (half * steps + j) * part
        return slice(start, start + part)

    for j in range(steps):
        first.put_z(j, ffn[:, feature(0, j)])
        first.put_p(j, ffn[:, feature(1, j)])

    @pl.loop(1, n)
    def _(d):
        message_copy(d, True).wait_recv()

    names = iota((n, 1), 0).astype(f32)
    left, right = iota((lane, 2 * lane), 0), iota((lane, 2 * lane), 1)
    ladder = jnp.where((left < right) | (right >= lane), 1.0, 0.0).astype(bf16)
    batch = min(n, max(1, 1024 // n))
    base[...] = jnp.zeros(base.shape, f32)

    def rank_batch(b):
        tiles = [mall[:, lanes(b * batch + i)] for i in range(batch)]
        hot = [[jnp.where(v[k : k + 1] == names, 1.0, 0.0) for k in range(top)] for v in tiles]
        counts = jnp.dot(
            jnp.concatenate([sum(h) for h in hot], axis=0).astype(bf16), ladder,
            preferred_element_type=f32,
        )
        running = base[...]
        for i in range(batch):
            count = counts[i * n : (i + 1) * n]
            place = running + count[:, :lane]
            running = running + count[:, lane:]
            raw = [tiles[i][top + k : top + k + 1] for k in range(top)]
            for k in range(top):
                rank = jnp.sum(hot[i][k] * place, axis=0, keepdims=True)
                code = jnp.where(rank < limit, tiles[i][k : k + 1] * limit + rank, -1.0)
                codes[k : k + 1, lanes(b * batch + i)] = code
                codes[top + k : top + k + 1, lanes(b * batch + i)] = raw[k] / sum(raw)
        base[...] = running

    if batch == n:
        rank_batch(0)
    else:
        pl.loop(0, n // batch)(rank_batch)

    def codes_of(devices):
        return jnp.concatenate([codes[:, lanes(d)][:, :rows] for d in devices], axis=1)

    def device_of(q, c, k):
        return q * group + c * cores + k

    along = [device_of(q, chip, k) for k in range(cores) for q in range(planes)]
    around = [device_of(plane, c, k) for k in range(cores) for c in range(chips)]
    mine_around = [device_of(plane, c, core) for c in range(chips)]
    mine_along = [device_of(q, chip, core) for q in range(planes)]

    def slots_of(devices, dim):
        spot = iota((1, rows) if dim else (rows, 1), dim)
        return jnp.concatenate([(d * limit + spot).astype(f32) for d in devices], axis=dim)

    def match(at_rows, at_lanes):
        hit = jnp.zeros((at_rows[0].shape[0], at_lanes[0].shape[1]), f32)
        for r in at_rows:
            for v in at_lanes:
                hit = jnp.where(r == v, 1.0, hit)
        return hit.astype(bf16)

    def split(block_of):
        return [block_of[k : k + 1] for k in range(top)]

    first.m2[...] = match([slots_of(mine_along, 0)], split(codes_of(around)))
    first.m1[...] = match([slots_of(mine_around, 0)], split(codes_of(along)))

    def fill_back():
        for m, targets, sources_of in (
            (second.m1, mine_around, along), (second.m2, mine_along, around)
        ):
            turned = jnp.transpose(codes_of(targets))
            m[...] = match(
                [turned[:, k : k + 1] for k in range(top)], [slots_of(sources_of, 1)]
            )
        share_at[...] = jnp.zeros(share_at.shape, f32)
        wanted = (me * limit + iota((rows, 1), 0)).astype(f32)

        def add_shares(b):
            found = share_at[...]
            for i in range(8):
                v = codes[:, lanes(b * 8 + i)]
                for k in range(top):
                    found = found + jnp.where(v[k : k + 1] == wanted, v[top + k : top + k + 1], 0.0)
            share_at[...] = found

        pl.loop(0, n // 8)(add_shares)

    started = [False]

    def absorb(half, j, x):
        if not started[0]:
            load["eg"].wait()
            load["eu"].wait()
        for w, sums in ((eg, sums_g), (eu, sums_u)):
            piece = jnp.dot(x, w[feature(half, j), :], preferred_element_type=f32)
            sums[...] = sums[...] + piece if started[0] else piece
        started[0] = True

    def take_z(j):
        absorb(0, j, first.z_take(j).astype(bf16))

    def take_p(j):
        first.p_take(j, total.at[0])
        absorb(1, j, total[0].astype(bf16))

    first.run(fill_back, take_z, take_p)

    hidden[...] = (jax.nn.silu(sums_g[...]) * sums_u[...]).astype(bf16)
    share = jnp.sum(share_at[...], axis=1, keepdims=True)
    load["ed"].wait()

    def expert_out(half, j):
        made = jnp.dot(hidden[...], ed[:, feature(half, j)], preferred_element_type=f32)
        return (made.astype(bf16).astype(f32) * share).astype(bf16)

    for j in range(steps):
        second.put_z(j, expert_out(0, j))
        second.put_p(j, expert_out(1, j))

    def keep_z(j):
        total[j] = second.z_take(j)

    def keep_p(j):
        second.p_take(j, total.at[steps + j])

    second.run(lambda: None, keep_z, keep_p)

    squares = jnp.zeros((rows, 1), f32)
    for c in range(2 * steps):
        squares = squares + jnp.sum(total[c] * total[c], axis=1, keepdims=True)
    scale = lax.rsqrt(squares / width + epsilon)
    for c in range(2 * steps):
        cols = slice(c * part, (c + 1) * part)
        out[:, cols] = (residual[:, cols] + total[c] * scale * g_out[:, cols]).astype(out.dtype)
    save_out = pltpu.make_async_copy(out, out_h, save_sem.at[2])
    save_out.start()

    @pl.loop(1, n)
    def _(d):
        message_copy(d, False).wait_send()

    first.drain()
    second.drain()
    save_branch.wait()
    save_state.wait()
    save_out.wait()


def finish_kernel(out_i, branch_i, state_i, conv_i, out_o, conv_o, state_o, ob, cb, sb, sems):
    past = conv_i.shape[0]
    ins = [
        pltpu.make_async_copy(conv_i.at[pl.ds(1, past - 1)], cb.at[pl.ds(0, past - 1)], sems.at[0]),
        pltpu.make_async_copy(branch_i, cb.at[past - 1], sems.at[1]),
        pltpu.make_async_copy(state_i, sb, sems.at[2]),
        pltpu.make_async_copy(out_i, ob, sems.at[3]),
    ]
    outs = [
        pltpu.make_async_copy(cb, conv_o, sems.at[4]),
        pltpu.make_async_copy(sb, state_o, sems.at[5]),
        pltpu.make_async_copy(ob, out_o, sems.at[6]),
    ]
    for copy in ins:
        copy.start()
    ins[0].wait()
    ins[1].wait()
    outs[0].start()
    ins[2].wait()
    outs[1].start()
    ins[3].wait()
    outs[2].start()
    for copy in outs:
        copy.wait()


def anywhere(count):
    return [pl.BlockSpec(memory_space=pl.ANY)] * count


def shards(
    tokens, conv_state, recur_state, w_branch, w_gate, conv_taps, rate_blocks, input_blocks,
    decay_param, w_mix, gain_pre, gain_post, gain_ffn, gain_out, routes, affinity,
    w_expert_gate, w_expert_up, w_expert_down,
):
    n = lax.axis_size("ep")
    rows, width = tokens.shape
    channels = recur_state.shape[1]
    past = conv_state.shape[1]
    top = routes.shape[1]
    ff = w_expert_gate.shape[2]
    block = rate_blocks.shape[2]
    limit = rows * top // 2
    assert limit == rows

    row = lambda v: v.reshape(1, -1)
    dma = lambda *count: pltpu.SemaphoreType.DMA(count)
    letter = (-(-2 * top // 8) * 8, lane)
    conv_turned = jnp.transpose(conv_state, (1, 0, 2))
    operands = (
        tokens, conv_turned, recur_state, w_branch, w_gate, conv_taps,
        rate_blocks.reshape(channels, block), input_blocks.reshape(channels, block),
        row(decay_param), w_mix, row(gain_pre), row(gain_post), row(gain_ffn), row(gain_out),
        routes.T, affinity.T, w_expert_gate, w_expert_up, w_expert_down,
    )
    held = [pltpu.VMEM(v.shape[1:] if k >= 16 else v.shape, v.dtype) for k, v in enumerate(operands)]
    made, branch, state = pl.pallas_call(
        functools.partial(layer_kernel, n, limit, top),
        out_shape=(
            jax.ShapeDtypeStruct((rows, width), bf16),
            jax.ShapeDtypeStruct((rows, channels), bf16),
            jax.ShapeDtypeStruct((rows, channels), f32),
        ),
        in_specs=anywhere(input_count),
        out_specs=tuple(anywhere(output_count)),
        scratch_shapes=held
        + exchange_scratch(n, rows, width)
        + exchange_scratch(n, rows, width)
        + [
            pltpu.VMEM((rows, width), bf16),
            pltpu.VMEM((rows, channels), bf16),
            pltpu.VMEM((rows, channels), f32),
            pltpu.VMEM((rows, width), bf16),
            pltpu.VMEM((rows, channels), bf16),
            pltpu.VMEM((rows, channels), bf16),
            pltpu.VMEM((rows, width), f32),
            pltpu.VMEM((rows, width), f32),
            pltpu.VMEM(letter, f32),
            pltpu.VMEM((letter[0], n * lane), f32),
            pltpu.VMEM((letter[0], n * lane), f32),
            pltpu.VMEM((n, lane), f32),
            pltpu.VMEM((rows, lane), f32),
            pltpu.VMEM((rows, ff), f32),
            pltpu.VMEM((rows, ff), f32),
            pltpu.VMEM((2 * steps, rows, width // (2 * steps)), f32),
            pltpu.VMEM((rows, ff), bf16),
            dma(16), dma((2 * channels + width) // tile), dma(3), dma(n), dma(n),
        ],
        compiler_params=pltpu.CompilerParams(
            collective_id=0, has_side_effects=True, vmem_limit_bytes=60 << 20
        ),
    )(*operands)
    layer_out, conv_next, state_next = pl.pallas_call(
        finish_kernel,
        out_shape=(
            jax.ShapeDtypeStruct((rows, width), bf16),
            jax.ShapeDtypeStruct((past, rows, channels), bf16),
            jax.ShapeDtypeStruct((rows, channels), f32),
        ),
        in_specs=anywhere(4),
        out_specs=tuple(anywhere(3)),
        scratch_shapes=[
            pltpu.VMEM((rows, width), bf16),
            pltpu.VMEM((past, rows, channels), bf16),
            pltpu.VMEM((rows, channels), f32),
            dma(7),
        ],
    )(made, branch, state, conv_turned)
    return (layer_out, jnp.transpose(conv_next, (1, 0, 2)), state_next)


def solution(mesh):
    ep, copied = "ep", P()
    return jax.shard_map(
        shards,
        mesh=mesh,
        in_specs=(P(ep, None), P(ep, None, None), P(ep, None))
        + (copied,) * 11
        + (P(ep, None),) * 2
        + (P(ep, None, None),) * 3,
        out_specs=(P(ep, None), P(ep, None, None), P(ep, None)),
        check_vma=False,
    )
```
